32 devices in a mesh: sp: 8 (over z, y), tp: 4 (over x, core).
Axes of the slice: x: 2, y: 2, z: 4, core: 2. Of those that a mesh axis runs over, the one named last changes fastest.
Arguments:
- tokens: bfloat16 [1536, 2048], P('sp'), may hold values from -10 to 10
- w_query: bfloat16 [2048, 1024], P(None, 'tp'), may hold values from -0.125 to 0.125
- w_key: bfloat16 [2048, 256], P(None, 'tp'), may hold values from -0.125 to 0.125
- w_value: bfloat16 [2048, 256], P(None, 'tp'), may hold values from -0.125 to 0.125
- w_output: bfloat16 [1024, 2048], P('tp'), may hold values from -0.1875 to 0.1875
- query_gain: float32 [64], replicated, may hold values from 0.4 to 9
- key_gain: float32 [64], replicated, may hold values from 0.4 to 9
Outputs:
- mixed_out: bfloat16 [1536, 2048], P(('sp', 'tp'))
- log_sums: float32 [16, 1536], P('tp', 'sp')
The draws below stay inside these ranges and needn't reach their ends.
All inputs are finite; a program needn't handle non-finite values.
Results may differ from the reference program's by a relative error of at most 0.009.
The reference program's roundings to bfloat16 on the way (of `weights` and `attended`) count: a program that leaves them out, or rounds other values in their place, can miss the bound.
Values may be sent and summed in bfloat16 or wider, within the bound.
A program may use at most 64 MiB of HBM per device.

```python
import math
import jax
import jax.numpy as jnp
from jax import lax

D = 2048
HEADS = 16
KV_HEADS = 4
HEAD = 64
GRID_W = 64
TOK_DEV = 192
TOKENS = 1536


def draw_tokens(key, part):
    first, second, third = jax.random.split(key, 3)
    n_blocks = TOKENS // TOK_DEV
    base = jax.random.normal(first, (TOKENS, D), jnp.float32)
    offsets = jax.random.uniform(second, (n_blocks, 1), jnp.float32, -0.5, 2.0)
    direction = jnp.clip(jax.random.normal(third, (1, D), jnp.float32), -3.0, 3.0)
    shifted = base + jnp.repeat(offsets, TOK_DEV, axis=0) * direction
    return jnp.clip(shifted, -10.0, 10.0).astype(jnp.bfloat16)


def gain_draw(key, salt):
    own = jax.random.fold_in(key, salt)
    base = 1.0 + 0.18 * jnp.clip(jax.random.normal(own, (HEAD,), jnp.float32), -3.0, 3.0)
    return base


def draw_query_gain(key, part):
    return gain_draw(key, 11)


def draw_key_gain(key, part):
    return gain_draw(key, 13)


def steps_of(stream_key, extent, cuts, smallest, largest):
    loudness = 1.0
    for dim, blocks in cuts:
        draws = jax.random.uniform(jax.random.fold_in(jax.random.fold_in(stream_key, 6), dim), (blocks,), jnp.float32, smallest / len(cuts), largest / len(cuts))
        loudness = loudness * jnp.repeat(jnp.exp(draws), extent[dim] // blocks).reshape((-1,) + (1,) * (len(extent) - 1 - dim))
    return loudness


def centred(stream_key, shape, spread, limit, cuts=(), held_as=jnp.bfloat16):
    factor_of = steps_of(stream_key, shape, cuts, -0.22, 0.18) if cuts else 1.0
    drawn = jax.random.normal(stream_key, shape, jnp.float32) * spread * factor_of
    return jnp.minimum(jnp.maximum(drawn, -limit), limit).astype(held_as)


def setup_inputs(seed: int = 0) -> dict:
    splits = jax.random.split(jax.random.key(seed), 8)
    tokens = draw_tokens(jax.random.fold_in(splits[7], 71), 0)
    w_query = centred(splits[1], (D, HEADS * HEAD), D ** -0.5, 0.125, ((1, 4),))
    w_key = centred(splits[2], (D, KV_HEADS * HEAD), D ** -0.5, 0.125, ((1, 4),))
    w_value = centred(splits[3], (D, KV_HEADS * HEAD), D ** -0.5, 0.125, ((1, 4),))
    w_output = centred(splits[4], (HEADS * HEAD, D), (HEADS * HEAD) ** -0.5, 0.1875, ((0, 4),))
    query_gain = draw_query_gain(jax.random.fold_in(splits[7], 71), 0)
    key_gain = draw_key_gain(jax.random.fold_in(splits[7], 71), 0)
    return dict(tokens=tokens, w_query=w_query, w_key=w_key, w_value=w_value, w_output=w_output, query_gain=query_gain, key_gain=key_gain)


ROPE_BASE = 10000.0
NORM_EPS = 1e-06

def rotate(values, position):
    dim = values.shape[-1]
    half_dim = dim // 2
    inverse = ROPE_BASE ** (-jnp.arange(half_dim, dtype=jnp.float32) * (2.0 / dim))
    angles = position.astype(jnp.float32)[:, None] * inverse[None, :]
    cosine = jnp.cos(angles)[:, None, :]
    sine = jnp.sin(angles)[:, None, :]
    first_half = values[..., :half_dim]
    second_half = values[..., half_dim:]
    return jnp.concatenate([first_half * cosine - second_half * sine, second_half * cosine + first_half * sine], -1)

def prepare(projected, gain_vec, grid_row, grid_col):
    values = projected.astype(jnp.float32)
    values = values * lax.rsqrt(lax.optimization_barrier(jnp.mean(values * values, -1, keepdims=True)) + NORM_EPS) * gain_vec
    split_at = values.shape[-1] // 2
    turned = jnp.concatenate([rotate(values[..., :split_at], grid_row), rotate(values[..., split_at:], grid_col)], -1)
    return turned.astype(jnp.bfloat16)

def reference(tokens, w_query, w_key, w_value, w_output, query_gain, key_gain):
    seq_len = tokens.shape[0]
    head_dim = query_gain.shape[0]
    query_raw = jnp.dot(tokens, w_query, preferred_element_type=jnp.float32).astype(jnp.bfloat16)
    key_raw = jnp.dot(tokens, w_key, preferred_element_type=jnp.float32).astype(jnp.bfloat16)
    value_raw = jnp.dot(tokens, w_value, preferred_element_type=jnp.float32).astype(jnp.bfloat16)
    positions = jnp.arange(seq_len, dtype=jnp.int32)
    grid_row = positions // GRID_W
    grid_col = positions % GRID_W
    queries = prepare(query_raw.reshape(seq_len, HEADS, head_dim), query_gain, grid_row, grid_col)
    key_rows = prepare(key_raw.reshape(seq_len, KV_HEADS, head_dim), key_gain, grid_row, grid_col)
    value_rows = value_raw.reshape(seq_len, KV_HEADS, head_dim).astype(jnp.float32)
    key_float = key_rows.astype(jnp.float32)
    group_size = HEADS // KV_HEADS
    block_len = math.gcd(seq_len, 256)
    n_blocks = seq_len // block_len
    query_blocks = queries.reshape(n_blocks, block_len, KV_HEADS, group_size, head_dim)
    score_scale = head_dim ** (-0.5)

    def one_block(query_block):
        scores = jnp.einsum('qkgd,skd->kgqs', query_block.astype(jnp.float32), key_float) * score_scale
        row_max = lax.optimization_barrier(jnp.max(scores, -1))
        expos = jnp.exp(scores - row_max[..., None])
        weight_sum = lax.optimization_barrier(jnp.sum(expos, -1))
        weights = expos.astype(jnp.bfloat16).astype(jnp.float32)
        summed = jnp.einsum('kgqs,skd->qkgd', weights, value_rows)
        summed = summed / jnp.transpose(weight_sum, (2, 0, 1))[..., None]
        attended_block = summed.astype(jnp.bfloat16).reshape(block_len, HEADS * head_dim)
        log_block = (row_max + jnp.log(weight_sum)).reshape(HEADS, block_len)
        return (attended_block, log_block)
    attended_all, log_all = lax.map(one_block, query_blocks)
    attended = attended_all.reshape(seq_len, HEADS * head_dim)
    log_sums = jnp.transpose(log_all, (1, 0, 2)).reshape(HEADS, seq_len)
    mixed_out = jnp.dot(attended, w_output, preferred_element_type=jnp.float32).astype(jnp.bfloat16)
    return (mixed_out, log_sums)
```

```python
import functools
import math

import jax
import jax.numpy as jnp
from jax import lax
from jax.experimental import pallas as pl
from jax.experimental.pallas import tpu as pltpu
from jax.sharding import PartitionSpec as P

GRID_W = 64
ROPE_BASE = 10000.0
NORM_EPS = 1e-06
CHUNKS = 4
MESH = pl.DeviceIdType.MESH
F32 = jnp.float32
BF16 = jnp.bfloat16


def column(row_vec):
    n = row_vec.shape[1]
    down = lax.broadcasted_iota(jnp.int32, (n, n), 0)
    across = lax.broadcasted_iota(jnp.int32, (n, n), 1)
    spread = jnp.where(down == across, jnp.broadcast_to(row_vec, (n, n)), 0.0)
    return jnp.sum(spread, axis=1, keepdims=True)


def tables(first, rows, copies, half):
    shape = (half, copies * rows)
    lane = lax.broadcasted_iota(jnp.int32, shape, 1)
    for c in range(copies - 1, 0, -1):
        lane = jnp.where(lane >= c * rows, lane - c * rows, lane) if c == 1 else jnp.where(
            lane >= c * rows, lane - (c - 1) * rows, lane
        )
    position = lane + first
    index = lax.broadcasted_iota(jnp.int32, shape, 0).astype(F32)
    inverse = jnp.exp(index * (-math.log(ROPE_BASE) / half))
    shift = GRID_W.bit_length() - 1
    row = lax.shift_right_logical(position, shift).astype(F32) * inverse
    col = jnp.bitwise_and(position, GRID_W - 1).astype(F32) * inverse
    return jnp.cos(row), jnp.sin(row), jnp.cos(col), jnp.sin(col)


def prepare(values, gain_col, tabs):
    head = values.shape[0]
    w = head // 4
    values = values * lax.rsqrt(jnp.mean(values * values, 0, keepdims=True) + NORM_EPS) * gain_col
    cr, sr, cc, sc = tabs
    a, b, c, d = (values[i * w : (i + 1) * w] for i in range(4))
    return jnp.concatenate(
        [a * cr - b * sr, b * cr + a * sr, c * cc - d * sc, d * cc + c * sc], axis=0
    )


def kernel(
    n_sp, n_tp,
    tok_hbm, wq_hbm, wk_hbm, wv_hbm, wo_hbm, qg_ref, kg_ref,
    out_ref, lse_ref,
    tok, wq, wk, wv, wo, kv_own, kvbuf, qpad, att, send_a, recv_a, keep, send_b, recv_b,
    load_sem, send_sem, fwd_sem, recv_sem, a_send, a_recv, b_send, b_recv,
):
    rows = tok.shape[0]
    head = wk.shape[1]
    heads = wq.shape[1] // head
    lanes = heads * rows
    width = wo.shape[1]
    chunk = width // CHUNKS
    part = rows // n_tp
    n_out = n_sp // 2

    me = lax.axis_index("sp")
    t = lax.axis_index("tp")
    outer = me // 2
    minor = me % 2
    partner = outer * 2 + 1 - minor
    tp_near = t + 1 - 2 * (t % 2)
    tp_far = (t + 2) % 4

    def peer(d):
        return ((outer + d) % n_out) * 2 + minor

    def origin(d):
        return (outer + n_out - d) % n_out

    loads = [
        pltpu.make_async_copy(src, dst, load_sem.at[i])
        for i, (src, dst) in enumerate(
            [(tok_hbm, tok), (wk_hbm, wk), (wv_hbm, wv), (wq_hbm, wq), (wo_hbm, wo)]
        )
    ]
    for load in loads[:4]:
        load.start()

    barrier = pltpu.get_barrier_semaphore()
    pl.semaphore_signal(barrier, inc=1, device_id={"sp": partner}, device_id_type=MESH)
    pl.semaphore_signal(barrier, inc=1, device_id={"tp": tp_near}, device_id_type=MESH)
    pl.semaphore_signal(barrier, inc=1, device_id={"tp": tp_far}, device_id_type=MESH)

    def greet(d, unused):
        pl.semaphore_signal(barrier, inc=1, device_id={"sp": peer(d)}, device_id_type=MESH)
        return unused

    lax.fori_loop(1, n_out, greet, 0)

    tabs = tables(me * rows, rows, heads, head // 4)
    key_tabs = tuple(x[:, :rows] for x in tabs)
    gain_q = column(qg_ref[...]) * (head ** -0.5)
    gain_k = column(kg_ref[...])

    loads[0].wait()
    loads[1].wait()
    loads[2].wait()
    loads[4].start()
    w_kv = jnp.concatenate([wv[...], wk[...]], axis=1)
    raw = jnp.dot(tok[...], w_kv, preferred_element_type=F32).astype(BF16).astype(F32)
    raw_t = raw.T
    keys_t = prepare(raw_t[head:], gain_k, key_tabs)
    kv_own[...] = jnp.concatenate([raw_t[:head], keys_t], axis=0).T.astype(BF16)

    def slot(i):
        return kvbuf.at[pl.ds(pl.multiple_of(i * rows, 16), rows), :]

    def to_partner():
        return pltpu.make_async_remote_copy(
            src_ref=kv_own, dst_ref=slot(me), send_sem=send_sem.at[0], recv_sem=recv_sem.at[me],
            device_id={"sp": partner}, device_id_type=MESH,
        )

    def to_peer(d):
        return pltpu.make_async_remote_copy(
            src_ref=kv_own, dst_ref=slot(me), send_sem=send_sem.at[d], recv_sem=recv_sem.at[me],
            device_id={"sp": peer(d)}, device_id_type=MESH,
        )

    def forward(d):
        i = origin(d) * 2 + minor
        return pltpu.make_async_remote_copy(
            src_ref=slot(i), dst_ref=slot(i), send_sem=fwd_sem.at[d], recv_sem=recv_sem.at[i],
            device_id={"sp": partner}, device_id_type=MESH,
        )

    def arrival(i):
        pltpu.make_async_remote_copy(
            src_ref=slot(i), dst_ref=slot(i), send_sem=send_sem.at[0], recv_sem=recv_sem.at[i],
            device_id={"sp": partner}, device_id_type=MESH,
        ).wait_recv()
        return kvbuf[pl.ds(pl.multiple_of(i * rows, 16), rows), :]

    pl.semaphore_wait(barrier, n_out + 2)

    def send_peer(d, unused):
        to_peer(d).start()
        return unused

    lax.fori_loop(1, n_out, send_peer, 0)
    to_partner().start()

    loads[3].wait()
    raw_q = jnp.dot(tok[...], wq[...], preferred_element_type=F32).astype(BF16).astype(F32)
    stacked = jnp.concatenate([raw_q[:, h * head : (h + 1) * head] for h in range(heads)], axis=0)
    queries = prepare(stacked.T, gain_q, tabs)
    qpad[...] = jnp.concatenate([jnp.zeros_like(queries), queries], axis=0).astype(BF16)

    def attend(kv, state):
        scores = jnp.dot(kv, qpad[...], preferred_element_type=F32)
        top = jnp.max(scores, axis=0, keepdims=True)
        if state is not None:
            top = jnp.maximum(top, state[0])
        expos = jnp.exp(scores - top)
        total = jnp.sum(expos, axis=0, keepdims=True)
        summed = lax.dot_general(
            kv[:, :head], expos.astype(BF16), (((0,), (0,)), ((), ())), preferred_element_type=F32
        )
        if state is not None:
            shrink = jnp.exp(state[0] - top)
            total = total + state[1] * shrink
            summed = summed + state[2] * shrink
        return top, total, summed

    state = attend(kv_own[...], None)
    state = attend(arrival(partner), state)

    def take_direct(d, state):
        i = origin(d) * 2 + minor
        block = arrival(i)
        forward(d).start()
        return attend(block, state)

    def take_forwarded(d, state):
        return attend(arrival(origin(d) * 2 + 1 - minor), state)

    if n_out <= 8:
        for d in range(1, n_out):
            state = take_direct(d, state)
        for d in range(1, n_out):
            state = take_forwarded(d, state)
    else:
        state = lax.fori_loop(1, n_out, take_direct, state)
        state = lax.fori_loop(1, n_out, take_forwarded, state)
    top, total, summed = state

    result = (summed / total).T.astype(BF16)
    att[...] = jnp.concatenate([result[h * rows : (h + 1) * rows] for h in range(heads)], axis=1)

    def rows_of(j):
        return att[pl.ds(pl.multiple_of(j * part, 16), part), :]

    side, side_minor = t // 2, t % 2
    give = jnp.concatenate(
        [rows_of((1 - side) * 2 + 1 - side_minor), rows_of(side * 2 + 1 - side_minor)], axis=0
    )
    hold = jnp.concatenate([rows_of((1 - side) * 2 + side_minor), rows_of(t)], axis=0)

    loads[4].wait()

    def copy_a(c):
        return pltpu.make_async_remote_copy(
            src_ref=send_a.at[c], dst_ref=recv_a.at[c], send_sem=a_send.at[c], recv_sem=a_recv.at[c],
            device_id={"tp": tp_near}, device_id_type=MESH,
        )

    def copy_b(c):
        return pltpu.make_async_remote_copy(
            src_ref=send_b.at[c], dst_ref=recv_b.at[c], send_sem=b_send.at[c], recv_sem=b_recv.at[c],
            device_id={"tp": tp_far}, device_id_type=MESH,
        )

    for c in range(CHUNKS):
        cols = slice(c * chunk, (c + 1) * chunk)
        send_a[c] = jnp.dot(give, wo[:, cols], preferred_element_type=F32).astype(BF16)
        copy_a(c).start()
    for c in range(CHUNKS):
        cols = slice(c * chunk, (c + 1) * chunk)
        mine = jnp.dot(hold, wo[:, cols], preferred_element_type=F32)
        copy_a(c).wait_recv()
        mine = mine + recv_a[c].astype(F32)
        send_b[c] = mine[:part].astype(BF16)
        copy_b(c).start()
        keep[c] = mine[part:]

    logs = top + jnp.log(total)
    for h in range(heads):
        lse_ref[h : h + 1, :] = logs[:, h * rows : (h + 1) * rows]

    for c in range(CHUNKS):
        cols = slice(c * chunk, (c + 1) * chunk)
        copy_b(c).wait_recv()
        out_ref[:, cols] = (keep[c] + recv_b[c].astype(F32)).astype(BF16)

    def drain(d, unused):
        to_peer(d).wait_send()
        forward(d).wait_send()
        return unused

    lax.fori_loop(1, n_out, drain, 0)
    to_partner().wait_send()
    for c in range(CHUNKS):
        copy_a(c).wait_send()
        copy_b(c).wait_send()


def solution(mesh):
    n_sp, n_tp = mesh.shape["sp"], mesh.shape["tp"]

    def shards(tokens, w_query, w_key, w_value, w_output, query_gain, key_gain):
        rows, depth = tokens.shape
        n_query, n_key = w_query.shape[1], w_key.shape[1]
        head = query_gain.shape[0]
        heads = n_query // head
        width = w_output.shape[1]
        part = rows // n_tp
        chunk = width // CHUNKS
        n_out = n_sp // 2
        hbm = pl.BlockSpec(memory_space=pl.ANY)
        vmem = pl.BlockSpec(memory_space=pltpu.VMEM)
        dma = pltpu.SemaphoreType.DMA
        return pl.pallas_call(
            functools.partial(kernel, n_sp, n_tp),
            out_shape=(
                jax.ShapeDtypeStruct((part, width), BF16),
                jax.ShapeDtypeStruct((heads, rows), F32),
            ),
            in_specs=[hbm] * 5 + [vmem] * 2,
            out_specs=(vmem, vmem),
            scratch_shapes=[
                pltpu.VMEM((rows, depth), BF16),
                pltpu.VMEM((depth, n_query), BF16),
                pltpu.VMEM((depth, n_key), BF16),
                pltpu.VMEM((depth, n_key), BF16),
                pltpu.VMEM((n_query, width), BF16),
                pltpu.VMEM((rows, 2 * head), BF16),
                pltpu.VMEM((n_sp * rows, 2 * head), BF16),
                pltpu.VMEM((2 * head, heads * rows), BF16),
                pltpu.VMEM((rows, n_query), BF16),
                pltpu.VMEM((CHUNKS, 2 * part, chunk), BF16),
                pltpu.VMEM((CHUNKS, 2 * part, chunk), BF16),
                pltpu.VMEM((CHUNKS, part, chunk), F32),
                pltpu.VMEM((CHUNKS, part, chunk), BF16),
                pltpu.VMEM((CHUNKS, part, chunk), BF16),
                dma((5,)),
                dma((n_out,)),
                dma((n_out,)),
                dma((n_sp,)),
                dma((CHUNKS,)),
                dma((CHUNKS,)),
                dma((CHUNKS,)),
                dma((CHUNKS,)),
            ],
            compiler_params=pltpu.CompilerParams(collective_id=0, has_side_effects=True),
            name="layer",
        )(tokens, w_query, w_key, w_value, w_output, query_gain[None, :], key_gain[None, :])

    placed = (P("sp", None), P(None, "tp"), P(None, "tp"), P(None, "tp"), P("tp", None), P(), P())
    return jax.shard_map(
        shards,
        mesh=mesh,
        in_specs=placed,
        out_specs=(P(("sp", "tp"), None), P("tp", "sp")),
        check_vma=False,
    )
```

```python
import functools
import math

import jax
import jax.numpy as jnp
from jax import lax
from jax.experimental import pallas as pl
from jax.experimental.pallas import tpu as pltpu
from jax.sharding import PartitionSpec as P

GRID_W = 64
ROPE_BASE = 10000.0
NORM_EPS = 1e-06
CHUNKS = 4
MESH = pl.DeviceIdType.MESH
F32 = jnp.float32
BF16 = jnp.bfloat16


def column(row_vec):
    n = row_vec.shape[1]
    down = lax.broadcasted_iota(jnp.int32, (n, n), 0)
    across = lax.broadcasted_iota(jnp.int32, (n, n), 1)
    spread = jnp.where(down == across, jnp.broadcast_to(row_vec, (n, n)), 0.0)
    return jnp.sum(spread, axis=1, keepdims=True)


def tables(first, rows, copies, half):
    shape = (half, copies * rows)
    lane = lax.broadcasted_iota(jnp.int32, shape, 1)
    for c in range(copies - 1, 0, -1):
        lane = jnp.where(lane >= c * rows, lane - c * rows, lane) if c == 1 else jnp.where(
            lane >= c * rows, lane - (c - 1) * rows, lane
        )
    position = lane + first
    index = lax.broadcasted_iota(jnp.int32, shape, 0).astype(F32)
    inverse = jnp.exp(index * (-math.log(ROPE_BASE) / half))
    shift = GRID_W.bit_length() - 1
    row = lax.shift_right_logical(position, shift).astype(F32) * inverse
    col = jnp.bitwise_and(position, GRID_W - 1).astype(F32) * inverse
    return jnp.cos(row), jnp.sin(row), jnp.cos(col), jnp.sin(col)


def prepare(values, gain_col, tabs):
    head = values.shape[0]
    w = head // 4
    values = values * lax.rsqrt(jnp.mean(values * values, 0, keepdims=True) + NORM_EPS) * gain_col
    cr, sr, cc, sc = tabs
    a, b, c, d = (values[i * w : (i + 1) * w] for i in range(4))
    return jnp.concatenate(
        [a * cr - b * sr, b * cr + a * sr, c * cc - d * sc, d * cc + c * sc], axis=0
    )


def kernel(
    n_sp, n_tp,
    tok_hbm, wq_hbm, wk_hbm, wv_hbm, wo_hbm, qg_ref, kg_ref,
    out_ref, lse_ref,
    tok, wq, w_kv, wo, kv_own, kvbuf, qpad, att, send_a, recv_a, keep, send_b, recv_b,
    load_sem, send_sem, fwd_sem, recv_sem, a_send, a_recv, b_send, b_recv,
):
    rows = tok.shape[0]
    head = w_kv.shape[0] // 2
    heads = wq.shape[1] // head
    lanes = heads * rows
    width = wo.shape[1]
    chunk = width // CHUNKS
    part = rows // n_tp
    n_out = n_sp // 2

    me = lax.axis_index("sp")
    t = lax.axis_index("tp")
    outer = me // 2
    minor = me % 2
    partner = outer * 2 + 1 - minor
    tp_near = t + 1 - 2 * (t % 2)
    tp_far = (t + 2) % 4

    def peer(d):
        return ((outer + d) % n_out) * 2 + minor

    def origin(d):
        return (outer + n_out - d) % n_out

    loads = [
        pltpu.make_async_copy(src, dst, load_sem.at[i])
        for i, (src, dst) in enumerate(
            [
                (tok_hbm, tok), (wv_hbm, w_kv.at[:head]), (wk_hbm, w_kv.at[head:]),
                (wq_hbm, wq), (wo_hbm, wo),
            ]
        )
    ]
    for load in loads[:4]:
        load.start()

    barrier = pltpu.get_barrier_semaphore()
    pl.semaphore_signal(barrier, inc=1, device_id={"sp": partner}, device_id_type=MESH)
    pl.semaphore_signal(barrier, inc=1, device_id={"tp": tp_near}, device_id_type=MESH)
    pl.semaphore_signal(barrier, inc=1, device_id={"tp": tp_far}, device_id_type=MESH)

    def greet(d, unused):
        pl.semaphore_signal(barrier, inc=1, device_id={"sp": peer(d)}, device_id_type=MESH)
        return unused

    lax.fori_loop(1, n_out, greet, 0)

    tabs = tables(me * rows, rows, heads, head // 4)
    key_tabs = tuple(x[:, :rows] for x in tabs)
    gain_q = column(qg_ref[...]) * (head ** -0.5)
    gain_k = column(kg_ref[...])

    loads[0].wait()
    loads[1].wait()
    loads[2].wait()
    loads[4].start()
    raw_t = lax.dot_general(
        w_kv[...], tok[...], (((1,), (1,)), ((), ())), preferred_element_type=F32
    ).astype(BF16).astype(F32)
    keys_t = prepare(raw_t[head:], gain_k, key_tabs)
    kv_own[...] = jnp.concatenate([raw_t[:head], keys_t], axis=0).T.astype(BF16)

    def slot(i):
        return kvbuf.at[pl.ds(pl.multiple_of(i * rows, 16), rows), :]

    def to_partner():
        return pltpu.make_async_remote_copy(
            src_ref=kv_own, dst_ref=slot(me), send_sem=send_sem.at[0], recv_sem=recv_sem.at[me],
            device_id={"sp": partner}, device_id_type=MESH,
        )

    def to_peer(d):
        return pltpu.make_async_remote_copy(
            src_ref=kv_own, dst_ref=slot(me), send_sem=send_sem.at[d], recv_sem=recv_sem.at[me],
            device_id={"sp": peer(d)}, device_id_type=MESH,
        )

    def forward(d):
        i = origin(d) * 2 + minor
        return pltpu.make_async_remote_copy(
            src_ref=slot(i), dst_ref=slot(i), send_sem=fwd_sem.at[d], recv_sem=recv_sem.at[i],
            device_id={"sp": partner}, device_id_type=MESH,
        )

    def arrival(i):
        pltpu.make_async_remote_copy(
            src_ref=slot(i), dst_ref=slot(i), send_sem=send_sem.at[0], recv_sem=recv_sem.at[i],
            device_id={"sp": partner}, device_id_type=MESH,
        ).wait_recv()
        return kvbuf[pl.ds(pl.multiple_of(i * rows, 16), rows), :]

    pl.semaphore_wait(barrier, n_out + 2)

    def send_peer(d, unused):
        to_peer(d).start()
        return unused

    lax.fori_loop(1, n_out, send_peer, 0)
    to_partner().start()

    loads[3].wait()
    raw_q = jnp.dot(tok[...], wq[...], preferred_element_type=F32).astype(BF16).astype(F32)
    stacked = jnp.concatenate([raw_q[:, h * head : (h + 1) * head] for h in range(heads)], axis=0)
    queries = prepare(stacked.T, gain_q, tabs)
    qpad[...] = jnp.concatenate([jnp.zeros_like(queries), queries], axis=0).astype(BF16)

    def attend(kv, state):
        scores = jnp.dot(kv, qpad[...], preferred_element_type=F32)
        top = jnp.max(scores, axis=0, keepdims=True)
        if state is not None:
            top = jnp.maximum(top, state[0])
        expos = jnp.exp(scores - top)
        total = jnp.sum(expos, axis=0, keepdims=True)
        summed = lax.dot_general(
            kv[:, :head], expos.astype(BF16), (((0,), (0,)), ((), ())), preferred_element_type=F32
        )
        if state is not None:
            shrink = jnp.exp(state[0] - top)
            total = total + state[1] * shrink
            summed = summed + state[2] * shrink
        return top, total, summed

    state = attend(kv_own[...], None)
    state = attend(arrival(partner), state)

    def take_direct(d, state):
        i = origin(d) * 2 + minor
        block = arrival(i)
        forward(d).start()
        return attend(block, state)

    def take_forwarded(d, state):
        return attend(arrival(origin(d) * 2 + 1 - minor), state)

    if n_out <= 8:
        for d in range(1, n_out):
            state = take_direct(d, state)
        for d in range(1, n_out):
            state = take_forwarded(d, state)
    else:
        state = lax.fori_loop(1, n_out, take_direct, state)
        state = lax.fori_loop(1, n_out, take_forwarded, state)
    top, total, summed = state

    result = (summed / total).T.astype(BF16)
    att[...] = jnp.concatenate([result[h * rows : (h + 1) * rows] for h in range(heads)], axis=1)

    def rows_of(j):
        return att[pl.ds(pl.multiple_of(j * part, 16), part), :]

    side, side_minor = t // 2, t % 2
    give = jnp.concatenate(
        [rows_of((1 - side) * 2 + 1 - side_minor), rows_of(side * 2 + 1 - side_minor)], axis=0
    )
    hold = jnp.concatenate([rows_of((1 - side) * 2 + side_minor), rows_of(t)], axis=0)

    loads[4].wait()

    def copy_a(c):
        return pltpu.make_async_remote_copy(
            src_ref=send_a.at[c], dst_ref=recv_a.at[c], send_sem=a_send.at[c], recv_sem=a_recv.at[c],
            device_id={"tp": tp_near}, device_id_type=MESH,
        )

    def copy_b(c):
        return pltpu.make_async_remote_copy(
            src_ref=send_b.at[c], dst_ref=recv_b.at[c], send_sem=b_send.at[c], recv_sem=b_recv.at[c],
            device_id={"tp": tp_far}, device_id_type=MESH,
        )

    for c in range(CHUNKS):
        cols = slice(c * chunk, (c + 1) * chunk)
        send_a[c] = jnp.dot(give, wo[:, cols], preferred_element_type=F32).astype(BF16)
        copy_a(c).start()
    for c in range(CHUNKS):
        cols = slice(c * chunk, (c + 1) * chunk)
        mine = jnp.dot(hold, wo[:, cols], preferred_element_type=F32)
        copy_a(c).wait_recv()
        mine = mine + recv_a[c].astype(F32)
        send_b[c] = mine[:part].astype(BF16)
        copy_b(c).start()
        keep[c] = mine[part:]

    logs = top + jnp.log(total)
    for h in range(heads):
        lse_ref[h : h + 1, :] = logs[:, h * rows : (h + 1) * rows]

    for c in range(CHUNKS):
        cols = slice(c * chunk, (c + 1) * chunk)
        copy_b(c).wait_recv()
        out_ref[:, cols] = (keep[c] + recv_b[c].astype(F32)).astype(BF16)

    def drain(d, unused):
        to_peer(d).wait_send()
        forward(d).wait_send()
        return unused

    lax.fori_loop(1, n_out, drain, 0)
    to_partner().wait_send()
    for c in range(CHUNKS):
        copy_a(c).wait_send()
        copy_b(c).wait_send()


def solution(mesh):
    n_sp, n_tp = mesh.shape["sp"], mesh.shape["tp"]

    def shards(tokens, w_query, w_key, w_value, w_output, query_gain, key_gain):
        rows, depth = tokens.shape
        n_query, n_key = w_query.shape[1], w_key.shape[1]
        head = query_gain.shape[0]
        heads = n_query // head
        width = w_output.shape[1]
        part = rows // n_tp
        chunk = width // CHUNKS
        n_out = n_sp // 2
        hbm = pl.BlockSpec(memory_space=pltpu.HBM)
        vmem = pl.BlockSpec(memory_space=pltpu.VMEM)
        dma = pltpu.SemaphoreType.DMA
        return pl.pallas_call(
            functools.partial(kernel, n_sp, n_tp),
            out_shape=(
                jax.ShapeDtypeStruct((part, width), BF16),
                jax.ShapeDtypeStruct((heads, rows), F32),
            ),
            in_specs=[hbm] * 5 + [vmem] * 2,
            out_specs=(vmem, vmem),
            scratch_shapes=[
                pltpu.VMEM((rows, depth), BF16),
                pltpu.VMEM((depth, n_query), BF16),
                pltpu.VMEM((2 * n_key, depth), BF16),
                pltpu.VMEM((n_query, width), BF16),
                pltpu.VMEM((rows, 2 * head), BF16),
                pltpu.VMEM((n_sp * rows, 2 * head), BF16),
                pltpu.VMEM((2 * head, heads * rows), BF16),
                pltpu.VMEM((rows, n_query), BF16),
                pltpu.VMEM((CHUNKS, 2 * part, chunk), BF16),
                pltpu.VMEM((CHUNKS, 2 * part, chunk), BF16),
                pltpu.VMEM((CHUNKS, part, chunk), F32),
                pltpu.VMEM((CHUNKS, part, chunk), BF16),
                pltpu.VMEM((CHUNKS, part, chunk), BF16),
                dma((5,)),
                dma((n_out,)),
                dma((n_out,)),
                dma((n_sp,)),
                dma((CHUNKS,)),
                dma((CHUNKS,)),
                dma((CHUNKS,)),
                dma((CHUNKS,)),
            ],
            compiler_params=pltpu.CompilerParams(collective_id=0, has_side_effects=True, vmem_limit_bytes=24 * 2**20),
            name="layer",
        )(tokens, w_query, w_key.T, w_value.T, w_output, query_gain[None, :], key_gain[None, :])

    placed = (P("sp", None), P(None, "tp"), P(None, "tp"), P(None, "tp"), P("tp", None), P(), P())
    return jax.shard_map(
        shards,
        mesh=mesh,
        in_specs=placed,
        out_specs=(P(("sp", "tp"), None), P("tp", "sp")),
        check_vma=False,
    )
```

```python
import functools
import math

import jax
import jax.numpy as jnp
from jax import lax
from jax.experimental import pallas as pl
from jax.experimental.pallas import tpu as pltpu
from jax.sharding import PartitionSpec as P

GRID_W = 64
ROPE_BASE = 10000.0
NORM_EPS = 1e-06
CHUNKS = 4
MESH = pl.DeviceIdType.MESH
F32 = jnp.float32
BF16 = jnp.bfloat16


def column(row_vec):
    n = row_vec.shape[1]
    down = lax.broadcasted_iota(jnp.int32, (n, n), 0)
    across = lax.broadcasted_iota(jnp.int32, (n, n), 1)
    spread = jnp.where(down == across, jnp.broadcast_to(row_vec, (n, n)), 0.0)
    return jnp.sum(spread, axis=1, keepdims=True)


def tables(first, rows, copies, half):
    shape = (half, copies * rows)
    lane = lax.broadcasted_iota(jnp.int32, shape, 1)
    for c in range(copies - 1, 0, -1):
        lane = jnp.where(lane >= c * rows, lane - c * rows, lane) if c == 1 else jnp.where(
            lane >= c * rows, lane - (c - 1) * rows, lane
        )
    position = lane + first
    index = lax.broadcasted_iota(jnp.int32, shape, 0).astype(F32)
    inverse = jnp.exp(index * (-math.log(ROPE_BASE) / half))
    shift = GRID_W.bit_length() - 1
    row = lax.shift_right_logical(position, shift).astype(F32) * inverse
    col = jnp.bitwise_and(position, GRID_W - 1).astype(F32) * inverse
    return jnp.cos(row), jnp.sin(row), jnp.cos(col), jnp.sin(col)


def prepare(values, gain_col, tabs):
    head = values.shape[0]
    w = head // 4
    values = values * lax.rsqrt(jnp.mean(values * values, 0, keepdims=True) + NORM_EPS) * gain_col
    cr, sr, cc, sc = tabs
    a, b, c, d = (values[i * w : (i + 1) * w] for i in range(4))
    return jnp.concatenate(
        [a * cr - b * sr, b * cr + a * sr, c * cc - d * sc, d * cc + c * sc], axis=0
    )


def kernel(
    n_sp, n_tp,
    tok_hbm, wq_hbm, wk_hbm, wv_hbm, wo_hbm, qg_ref, kg_ref,
    out_ref, lse_ref,
    tok, wq, w_kv, wo, kv_own, kvbuf, qpad, att, send_a, recv_a, keep, send_b, recv_b,
    load_sem, send_sem, fwd_sem, recv_sem, a_send, a_recv, b_send, b_recv,
):
    rows = tok.shape[0]
    head = w_kv.shape[0] // 2
    heads = wq.shape[1] // head
    lanes = heads * rows
    width = wo.shape[1]
    chunk = width // CHUNKS
    part = rows // n_tp
    n_out = n_sp // 2

    me = lax.axis_index("sp")
    t = lax.axis_index("tp")
    outer = me // 2
    minor = me % 2
    partner = outer * 2 + 1 - minor
    tp_near = t + 1 - 2 * (t % 2)
    tp_far = (t + 2) % 4

    def peer(d):
        return ((outer + d) % n_out) * 2 + minor

    def origin(d):
        return (outer + n_out - d) % n_out

    loads = [
        pltpu.make_async_copy(src, dst, load_sem.at[i])
        for i, (src, dst) in enumerate(
            [
                (tok_hbm, tok), (wv_hbm, w_kv.at[:head]), (wk_hbm, w_kv.at[head:]),
                (wq_hbm, wq), (wo_hbm, wo),
            ]
        )
    ]
    for load in loads[:4]:
        load.start()

    barrier = pltpu.get_barrier_semaphore()
    pl.semaphore_signal(barrier, inc=1, device_id={"sp": partner}, device_id_type=MESH)
    pl.semaphore_signal(barrier, inc=1, device_id={"tp": tp_near}, device_id_type=MESH)
    pl.semaphore_signal(barrier, inc=1, device_id={"tp": tp_far}, device_id_type=MESH)

    def greet(d, unused):
        pl.semaphore_signal(barrier, inc=1, device_id={"sp": peer(d)}, device_id_type=MESH)
        return unused

    lax.fori_loop(1, n_out, greet, 0)

    tabs = tables(me * rows, rows, heads, head // 4)
    key_tabs = tuple(x[:, :rows] for x in tabs)
    gain_q = column(qg_ref[...]) * (head ** -0.5)
    gain_k = column(kg_ref[...])

    loads[0].wait()
    loads[1].wait()
    loads[2].wait()
    loads[4].start()
    raw_t = lax.dot_general(
        w_kv[...], tok[...], (((1,), (1,)), ((), ())), preferred_element_type=F32
    ).astype(BF16).astype(F32)
    keys_t = prepare(raw_t[head:], gain_k, key_tabs)
    kv_own[...] = jnp.concatenate([raw_t[:head], keys_t], axis=0).T.astype(BF16)

    def slot(i):
        return kvbuf.at[pl.ds(pl.multiple_of(i * rows, 16), rows), :]

    def to_partner():
        return pltpu.make_async_remote_copy(
            src_ref=kv_own, dst_ref=slot(me), send_sem=send_sem.at[0], recv_sem=recv_sem.at[me],
            device_id={"sp": partner}, device_id_type=MESH,
        )

    def to_peer(d):
        return pltpu.make_async_remote_copy(
            src_ref=kv_own, dst_ref=slot(me), send_sem=send_sem.at[d], recv_sem=recv_sem.at[me],
            device_id={"sp": peer(d)}, device_id_type=MESH,
        )

    def forward(d):
        i = origin(d) * 2 + minor
        return pltpu.make_async_remote_copy(
            src_ref=slot(i), dst_ref=slot(i), send_sem=fwd_sem.at[d], recv_sem=recv_sem.at[i],
            device_id={"sp": partner}, device_id_type=MESH,
        )

    def arrival(i):
        pltpu.make_async_remote_copy(
            src_ref=slot(i), dst_ref=slot(i), send_sem=send_sem.at[0], recv_sem=recv_sem.at[i],
            device_id={"sp": partner}, device_id_type=MESH,
        ).wait_recv()
        return kvbuf[pl.ds(pl.multiple_of(i * rows, 16), rows), :]

    pl.semaphore_wait(barrier, n_out + 2)

    def send_peer(d, unused):
        to_peer(d).start()
        return unused

    lax.fori_loop(1, n_out, send_peer, 0)
    to_partner().start()

    loads[3].wait()
    raw_q = jnp.dot(tok[...], wq[...], preferred_element_type=F32).astype(BF16).astype(F32)
    stacked = jnp.concatenate([raw_q[:, h * head : (h + 1) * head] for h in range(heads)], axis=0)
    queries = prepare(stacked.T, gain_q, tabs)
    qpad[...] = jnp.concatenate([jnp.zeros_like(queries), queries], axis=0).astype(BF16)

    def attend(kv, state):
        scores = jnp.dot(kv, qpad[...], preferred_element_type=F32)
        top = jnp.max(scores, axis=0, keepdims=True)
        if state is not None:
            top = jnp.maximum(top, state[0])
        expos = jnp.exp(scores - top)
        total = jnp.sum(expos, axis=0, keepdims=True)
        summed = lax.dot_general(
            kv[:, :head], expos.astype(BF16), (((0,), (0,)), ((), ())), preferred_element_type=F32
        )
        if state is not None:
            shrink = jnp.exp(state[0] - top)
            total = total + state[1] * shrink
            summed = summed + state[2] * shrink
        return top, total, summed

    state = attend(kv_own[...], None)
    state = attend(arrival(partner), state)

    def take_direct(d, state):
        i = origin(d) * 2 + minor
        block = arrival(i)
        forward(d).start()
        return attend(block, state)

    def take_forwarded(d, state):
        return attend(arrival(origin(d) * 2 + 1 - minor), state)

    if n_out <= 8:
        for d in range(1, n_out):
            state = take_direct(d, state)
        for d in range(1, n_out):
            state = take_forwarded(d, state)
    else:
        state = lax.fori_loop(1, n_out, take_direct, state)
        state = lax.fori_loop(1, n_out, take_forwarded, state)
    top, total, summed = state

    result = (summed / total).T.astype(BF16)
    att[...] = jnp.concatenate([result[h * rows : (h + 1) * rows] for h in range(heads)], axis=1)

    def rows_of(j):
        return att[pl.ds(pl.multiple_of(j * part, 16), part), :]

    side, side_minor = t // 2, t % 2
    give = jnp.concatenate(
        [rows_of((1 - side) * 2 + 1 - side_minor), rows_of(side * 2 + 1 - side_minor)], axis=0
    )
    hold = jnp.concatenate([rows_of((1 - side) * 2 + side_minor), rows_of(t)], axis=0)

    loads[4].wait()

    def copy_a(c):
        return pltpu.make_async_remote_copy(
            src_ref=send_a.at[c], dst_ref=recv_a.at[c], send_sem=a_send.at[c], recv_sem=a_recv.at[c],
            device_id={"tp": tp_near}, device_id_type=MESH,
        )

    def copy_b(c):
        return pltpu.make_async_remote_copy(
            src_ref=send_b.at[c], dst_ref=recv_b.at[c], send_sem=b_send.at[c], recv_sem=b_recv.at[c],
            device_id={"tp": tp_far}, device_id_type=MESH,
        )

    for c in range(CHUNKS):
        cols = slice(c * chunk, (c + 1) * chunk)
        send_a[c] = jnp.dot(give, wo[:, cols], preferred_element_type=F32).astype(BF16)
        copy_a(c).start()
    for c in range(CHUNKS):
        cols = slice(c * chunk, (c + 1) * chunk)
        mine = jnp.dot(hold, wo[:, cols], preferred_element_type=F32)
        copy_a(c).wait_recv()
        mine = mine + recv_a[c].astype(F32)
        send_b[c] = mine[:part].astype(BF16)
        copy_b(c).start()
        keep[c] = mine[part:]

    logs = top + jnp.log(total)
    for h in range(heads):
        lse_ref[h : h + 1, :] = logs[:, h * rows : (h + 1) * rows]

    for c in range(CHUNKS):
        cols = slice(c * chunk, (c + 1) * chunk)
        copy_b(c).wait_recv()
        out_ref[:, cols] = (keep[c] + recv_b[c].astype(F32)).astype(BF16)

    def drain(d, unused):
        to_peer(d).wait_send()
        forward(d).wait_send()
        return unused

    lax.fori_loop(1, n_out, drain, 0)
    to_partner().wait_send()
    for c in range(CHUNKS):
        copy_a(c).wait_send()
        copy_b(c).wait_send()


def solution(mesh):
    n_sp, n_tp = mesh.shape["sp"], mesh.shape["tp"]

    def shards(tokens, w_query, w_key, w_value, w_output, query_gain, key_gain):
        rows, depth = tokens.shape
        n_query, n_key = w_query.shape[1], w_key.shape[1]
        head = query_gain.shape[0]
        heads = n_query // head
        width = w_output.shape[1]
        part = rows // n_tp
        chunk = width // CHUNKS
        n_out = n_sp // 2
        hbm = pl.BlockSpec(memory_space=pl.ANY)
        vmem = pl.BlockSpec(memory_space=pltpu.VMEM)
        dma = pltpu.SemaphoreType.DMA
        return pl.pallas_call(
            functools.partial(kernel, n_sp, n_tp),
            out_shape=(
                jax.ShapeDtypeStruct((part, width), BF16),
                jax.ShapeDtypeStruct((heads, rows), F32),
            ),
            in_specs=[hbm] * 5 + [vmem] * 2,
            out_specs=(vmem, vmem),
            scratch_shapes=[
                pltpu.VMEM((rows, depth), BF16),
                pltpu.VMEM((depth, n_query), BF16),
                pltpu.VMEM((2 * n_key, depth), BF16),
                pltpu.VMEM((n_query, width), BF16),
                pltpu.VMEM((rows, 2 * head), BF16),
                pltpu.VMEM((n_sp * rows, 2 * head), BF16),
                pltpu.VMEM((2 * head, heads * rows), BF16),
                pltpu.VMEM((rows, n_query), BF16),
                pltpu.VMEM((CHUNKS, 2 * part, chunk), BF16),
                pltpu.VMEM((CHUNKS, 2 * part, chunk), BF16),
                pltpu.VMEM((CHUNKS, part, chunk), F32),
                pltpu.VMEM((CHUNKS, part, chunk), BF16),
                pltpu.VMEM((CHUNKS, part, chunk), BF16),
                dma((5,)),
                dma((n_out,)),
                dma((n_out,)),
                dma((n_sp,)),
                dma((CHUNKS,)),
                dma((CHUNKS,)),
                dma((CHUNKS,)),
                dma((CHUNKS,)),
            ],
            compiler_params=pltpu.CompilerParams(collective_id=0, has_side_effects=True),
            name="layer",
        )(tokens, w_query, w_key.T, w_value.T, w_output, query_gain[None, :], key_gain[None, :])

    placed = (P("sp", None), P(None, "tp"), P(None, "tp"), P(None, "tp"), P("tp", None), P(), P())
    return jax.shard_map(
        shards,
        mesh=mesh,
        in_specs=placed,
        out_specs=(P(("sp", "tp"), None), P("tp", "sp")),
        check_vma=False,
    )
```

```python
import functools
import math

import jax
import jax.numpy as jnp
from jax import lax
from jax.experimental import pallas as pl
from jax.experimental.pallas import tpu as pltpu
from jax.sharding import PartitionSpec as P

GRID_W = 64
ROPE_BASE = 10000.0
NORM_EPS = 1e-06
CHUNKS = 4
MESH = pl.DeviceIdType.MESH
F32 = jnp.float32
BF16 = jnp.bfloat16


def column(row_vec):
    n = row_vec.shape[1]
    down = lax.broadcasted_iota(jnp.int32, (n, n), 0)
    across = lax.broadcasted_iota(jnp.int32, (n, n), 1)
    spread = jnp.where(down == across, jnp.broadcast_to(row_vec, (n, n)), 0.0)
    return jnp.sum(spread, axis=1, keepdims=True)


def tables(first, rows, copies, half):
    shape = (half, copies * rows)
    lane = lax.broadcasted_iota(jnp.int32, shape, 1)
    for c in range(copies - 1, 0, -1):
        lane = jnp.where(lane >= c * rows, lane - c * rows, lane) if c == 1 else jnp.where(
            lane >= c * rows, lane - (c - 1) * rows, lane
        )
    position = lane + first
    index = lax.broadcasted_iota(jnp.int32, shape, 0).astype(F32)
    inverse = jnp.exp(index * (-math.log(ROPE_BASE) / half))
    shift = GRID_W.bit_length() - 1
    row = lax.shift_right_logical(position, shift).astype(F32) * inverse
    col = jnp.bitwise_and(position, GRID_W - 1).astype(F32) * inverse
    return jnp.cos(row), jnp.sin(row), jnp.cos(col), jnp.sin(col)


def prepare(values, gain_col, tabs):
    head = values.shape[0]
    w = head // 4
    values = values * lax.rsqrt(jnp.mean(values * values, 0, keepdims=True) + NORM_EPS) * gain_col
    cr, sr, cc, sc = tabs
    a, b, c, d = (values[i * w : (i + 1) * w] for i in range(4))
    return jnp.concatenate(
        [a * cr - b * sr, b * cr + a * sr, c * cc - d * sc, d * cc + c * sc], axis=0
    )


def kernel(
    n_sp, n_tp,
    tok_hbm, wq_hbm, wk_hbm, wv_hbm, wo_hbm, qg_hbm, kg_hbm,
    out_ref, lse_ref,
    tok, wq, w_kv, wo, qg_ref, kg_ref, kv_own, kvbuf, qpad, att, send_a, recv_a, keep, send_b, recv_b,
    load_sem, send_sem, fwd_sem, recv_sem, a_send, a_recv, b_send, b_recv,
):
    rows = tok.shape[0]
    head = w_kv.shape[0] // 2
    heads = wq.shape[1] // head
    lanes = heads * rows
    width = wo.shape[1]
    chunk = width // CHUNKS
    part = rows // n_tp
    n_out = n_sp // 2

    me = lax.axis_index("sp")
    t = lax.axis_index("tp")
    outer = me // 2
    minor = me % 2
    partner = outer * 2 + 1 - minor
    tp_near = t + 1 - 2 * (t % 2)
    tp_far = (t + 2) % 4

    def peer(d):
        return ((outer + d) % n_out) * 2 + minor

    def origin(d):
        return (outer + n_out - d) % n_out

    loads = [
        pltpu.make_async_copy(src, dst, load_sem.at[i])
        for i, (src, dst) in enumerate(
            [
                (tok_hbm, tok), (wv_hbm, w_kv.at[:head]), (wk_hbm, w_kv.at[head:]),
                (wq_hbm, wq), (wo_hbm, wo),
                (qg_hbm, qg_ref), (kg_hbm, kg_ref),
            ]
        )
    ]
    for load in loads[5:] + loads[:3]:
        load.start()

    barrier = pltpu.get_barrier_semaphore()
    pl.semaphore_signal(barrier, inc=1, device_id={"sp": partner}, device_id_type=MESH)
    pl.semaphore_signal(barrier, inc=1, device_id={"tp": tp_near}, device_id_type=MESH)
    pl.semaphore_signal(barrier, inc=1, device_id={"tp": tp_far}, device_id_type=MESH)

    def greet(d, unused):
        pl.semaphore_signal(barrier, inc=1, device_id={"sp": peer(d)}, device_id_type=MESH)
        return unused

    lax.fori_loop(1, n_out, greet, 0)

    tabs = tables(me * rows, rows, heads, head // 4)
    key_tabs = tuple(x[:, :rows] for x in tabs)
    loads[5].wait()
    loads[6].wait()
    gain_q = column(qg_ref[...]) * (head ** -0.5)
    gain_k = column(kg_ref[...])

    loads[0].wait()
    loads[1].wait()
    loads[2].wait()
    loads[3].start()
    loads[4].start()
    raw_t = lax.dot_general(
        w_kv[...], tok[...], (((1,), (1,)), ((), ())), preferred_element_type=F32
    ).astype(BF16).astype(F32)
    keys_t = prepare(raw_t[head:], gain_k, key_tabs)
    kv_own[...] = jnp.concatenate([raw_t[:head], keys_t], axis=0).T.astype(BF16)

    def slot(i):
        return kvbuf.at[pl.ds(pl.multiple_of(i * rows, 16), rows), :]

    def to_partner():
        return pltpu.make_async_remote_copy(
            src_ref=kv_own, dst_ref=slot(me), send_sem=send_sem.at[0], recv_sem=recv_sem.at[me],
            device_id={"sp": partner}, device_id_type=MESH,
        )

    def to_peer(d):
        return pltpu.make_async_remote_copy(
            src_ref=kv_own, dst_ref=slot(me), send_sem=send_sem.at[d], recv_sem=recv_sem.at[me],
            device_id={"sp": peer(d)}, device_id_type=MESH,
        )

    def forward(d):
        i = origin(d) * 2 + minor
        return pltpu.make_async_remote_copy(
            src_ref=slot(i), dst_ref=slot(i), send_sem=fwd_sem.at[d], recv_sem=recv_sem.at[i],
            device_id={"sp": partner}, device_id_type=MESH,
        )

    def land(i):
        pltpu.make_async_remote_copy(
            src_ref=slot(i), dst_ref=slot(i), send_sem=send_sem.at[0], recv_sem=recv_sem.at[i],
            device_id={"sp": partner}, device_id_type=MESH,
        ).wait_recv()

    def held(i):
        return kvbuf[pl.ds(pl.multiple_of(i * rows, 16), rows), :]

    def arrival(i):
        land(i)
        return held(i)

    pl.semaphore_wait(barrier, n_out + 2)

    def send_peer(d, unused):
        to_peer(d).start()
        return unused

    lax.fori_loop(1, n_out, send_peer, 0)
    to_partner().start()

    loads[3].wait()
    raw_q = jnp.dot(tok[...], wq[...], preferred_element_type=F32).astype(BF16).astype(F32)
    stacked = jnp.concatenate([raw_q[:, h * head : (h + 1) * head] for h in range(heads)], axis=0)
    queries = prepare(stacked.T, gain_q, tabs)
    qpad[...] = jnp.concatenate([jnp.zeros_like(queries), queries], axis=0).astype(BF16)

    def attend(kv, state):
        scores = jnp.dot(kv, qpad[...], preferred_element_type=F32)
        top = jnp.max(scores, axis=0, keepdims=True)
        if state is not None:
            top = jnp.maximum(top, state[0])
        expos = jnp.exp(scores - top)
        total = jnp.sum(expos, axis=0, keepdims=True)
        summed = lax.dot_general(
            kv[:, :head], expos.astype(BF16), (((0,), (0,)), ((), ())), preferred_element_type=F32
        )
        if state is not None:
            shrink = jnp.exp(state[0] - top)
            total = total + state[1] * shrink
            summed = summed + state[2] * shrink
        return top, total, summed

    state = attend(kv_own[...], None)

    def take_direct(d, state):
        i = origin(d) * 2 + minor
        block = arrival(i)
        forward(d).start()
        return attend(block, state)

    def take_forwarded(d, state):
        return attend(arrival(origin(d) * 2 + 1 - minor), state)

    if n_out <= 8:
        ready = partner
        for d in range(1, n_out):
            i = origin(d) * 2 + minor
            land(i)
            forward(d).start()
            if d == 1:
                land(partner)
            state = attend(held(ready), state)
            ready = i
        state = attend(held(ready), state)
        for d in range(1, n_out):
            state = take_forwarded(d, state)
    else:
        state = attend(arrival(partner), state)
        state = lax.fori_loop(1, n_out, take_direct, state)
        state = lax.fori_loop(1, n_out, take_forwarded, state)
    top, total, summed = state

    result = (summed / total).T.astype(BF16)
    att[...] = jnp.concatenate([result[h * rows : (h + 1) * rows] for h in range(heads)], axis=1)

    def rows_of(j):
        return att[pl.ds(pl.multiple_of(j * part, 16), part), :]

    side, side_minor = t // 2, t % 2
    give = jnp.concatenate(
        [rows_of((1 - side) * 2 + 1 - side_minor), rows_of(side * 2 + 1 - side_minor)], axis=0
    )
    hold = jnp.concatenate([rows_of((1 - side) * 2 + side_minor), rows_of(t)], axis=0)

    loads[4].wait()

    def copy_a(c):
        return pltpu.make_async_remote_copy(
            src_ref=send_a.at[c], dst_ref=recv_a.at[c], send_sem=a_send.at[c], recv_sem=a_recv.at[c],
            device_id={"tp": tp_near}, device_id_type=MESH,
        )

    def copy_b(c):
        return pltpu.make_async_remote_copy(
            src_ref=send_b.at[c], dst_ref=recv_b.at[c], send_sem=b_send.at[c], recv_sem=b_recv.at[c],
            device_id={"tp": tp_far}, device_id_type=MESH,
        )

    for c in range(CHUNKS):
        cols = slice(c * chunk, (c + 1) * chunk)
        send_a[c] = jnp.dot(give, wo[:, cols], preferred_element_type=F32).astype(BF16)
        copy_a(c).start()
    for c in range(CHUNKS):
        cols = slice(c * chunk, (c + 1) * chunk)
        mine = jnp.dot(hold, wo[:, cols], preferred_element_type=F32)
        copy_a(c).wait_recv()
        mine = mine + recv_a[c].astype(F32)
        send_b[c] = mine[:part].astype(BF16)
        copy_b(c).start()
        keep[c] = mine[part:]

    logs = top + jnp.log(total)
    for h in range(heads):
        lse_ref[h : h + 1, :] = logs[:, h * rows : (h + 1) * rows]

    for c in range(CHUNKS):
        cols = slice(c * chunk, (c + 1) * chunk)
        copy_b(c).wait_recv()
        out_ref[:, cols] = (keep[c] + recv_b[c].astype(F32)).astype(BF16)

    def drain(d, unused):
        to_peer(d).wait_send()
        forward(d).wait_send()
        return unused

    lax.fori_loop(1, n_out, drain, 0)
    to_partner().wait_send()
    for c in range(CHUNKS):
        copy_a(c).wait_send()
        copy_b(c).wait_send()


def solution(mesh):
    n_sp, n_tp = mesh.shape["sp"], mesh.shape["tp"]

    def shards(tokens, w_query, w_key, w_value, w_output, query_gain, key_gain):
        rows, depth = tokens.shape
        n_query, n_key = w_query.shape[1], w_key.shape[1]
        head = query_gain.shape[0]
        heads = n_query // head
        width = w_output.shape[1]
        part = rows // n_tp
        chunk = width // CHUNKS
        n_out = n_sp // 2
        hbm = pl.BlockSpec(memory_space=pl.ANY)
        vmem = pl.BlockSpec(memory_space=pltpu.VMEM)
        dma = pltpu.SemaphoreType.DMA
        def stay(x):
            return pltpu.with_memory_space_constraint(x, pltpu.HBM)

        return pl.pallas_call(
            functools.partial(kernel, n_sp, n_tp),
            out_shape=(
                jax.ShapeDtypeStruct((part, width), BF16),
                jax.ShapeDtypeStruct((heads, rows), F32),
            ),
            in_specs=[hbm] * 7,
            out_specs=(vmem, vmem),
            scratch_shapes=[
                pltpu.VMEM((rows, depth), BF16),
                pltpu.VMEM((depth, n_query), BF16),
                pltpu.VMEM((2 * n_key, depth), BF16),
                pltpu.VMEM((n_query, width), BF16),
                pltpu.VMEM((1, head), F32),
                pltpu.VMEM((1, head), F32),
                pltpu.VMEM((rows, 2 * head), BF16),
                pltpu.VMEM((n_sp * rows, 2 * head), BF16),
                pltpu.VMEM((2 * head, heads * rows), BF16),
                pltpu.VMEM((rows, n_query), BF16),
                pltpu.VMEM((CHUNKS, 2 * part, chunk), BF16),
                pltpu.VMEM((CHUNKS, 2 * part, chunk), BF16),
                pltpu.VMEM((CHUNKS, part, chunk), F32),
                pltpu.VMEM((CHUNKS, part, chunk), BF16),
                pltpu.VMEM((CHUNKS, part, chunk), BF16),
                dma((7,)),
                dma((n_out,)),
                dma((n_out,)),
                dma((n_sp,)),
                dma((CHUNKS,)),
                dma((CHUNKS,)),
                dma((CHUNKS,)),
                dma((CHUNKS,)),
            ],
            compiler_params=pltpu.CompilerParams(collective_id=0, has_side_effects=True, vmem_limit_bytes=32 * 2**20),
            name="layer",
        )(
            stay(tokens), stay(w_query), stay(w_key.T), stay(w_value.T), stay(w_output),
            stay(query_gain[None, :]), stay(key_gain[None, :]),
        )

    placed = (P("sp", None), P(None, "tp"), P(None, "tp"), P(None, "tp"), P("tp", None), P(), P())
    return jax.shard_map(
        shards,
        mesh=mesh,
        in_specs=placed,
        out_specs=(P(("sp", "tp"), None), P("tp", "sp")),
        check_vma=False,
    )
```

```python
import functools
import math

import jax
import jax.numpy as jnp
from jax import lax
from jax.experimental import pallas as pl
from jax.experimental.pallas import tpu as pltpu
from jax.sharding import PartitionSpec as P

GRID_W = 64
ROPE_BASE = 10000.0
NORM_EPS = 1e-06
CHUNKS = 4
MESH = pl.DeviceIdType.MESH
F32 = jnp.float32
BF16 = jnp.bfloat16


def column(row_vec):
    n = row_vec.shape[1]
    down = lax.broadcasted_iota(jnp.int32, (n, n), 0)
    across = lax.broadcasted_iota(jnp.int32, (n, n), 1)
    spread = jnp.where(down == across, jnp.broadcast_to(row_vec, (n, n)), 0.0)
    return jnp.sum(spread, axis=1, keepdims=True)


def tables(first, rows, copies, half):
    shape = (half, copies * rows)
    lane = lax.broadcasted_iota(jnp.int32, shape, 1)
    for c in range(copies - 1, 0, -1):
        lane = jnp.where(lane >= c * rows, lane - c * rows, lane) if c == 1 else jnp.where(
            lane >= c * rows, lane - (c - 1) * rows, lane
        )
    position = lane + first
    index = lax.broadcasted_iota(jnp.int32, shape, 0).astype(F32)
    inverse = jnp.exp(index * (-math.log(ROPE_BASE) / half))
    shift = GRID_W.bit_length() - 1
    row = lax.shift_right_logical(position, shift).astype(F32) * inverse
    col = jnp.bitwise_and(position, GRID_W - 1).astype(F32) * inverse
    return jnp.cos(row), jnp.sin(row), jnp.cos(col), jnp.sin(col)


def prepare(values, gain_col, tabs):
    head = values.shape[0]
    w = head // 4
    values = values * lax.rsqrt(jnp.mean(values * values, 0, keepdims=True) + NORM_EPS) * gain_col
    cr, sr, cc, sc = tabs
    a, b, c, d = (values[i * w : (i + 1) * w] for i in range(4))
    return jnp.concatenate(
        [a * cr - b * sr, b * cr + a * sr, c * cc - d * sc, d * cc + c * sc], axis=0
    )


def kernel(
    n_sp, n_tp,
    tok_hbm, wq_hbm, wk_hbm, wv_hbm, wo_hbm, qg_hbm, kg_hbm,
    out_ref, lse_ref,
    tok, wq, w_kv, wo, qg_ref, kg_ref, kv_own, kvbuf, qpad, att, send_a, recv_a, keep, send_b, recv_b,
    load_sem, send_sem, fwd_sem, recv_sem, a_send, a_recv, b_send, b_recv,
):
    rows = tok.shape[0]
    head = w_kv.shape[0] // 2
    heads = wq.shape[1] // head
    lanes = heads * rows
    width = wo.shape[1]
    chunk = width // CHUNKS
    part = rows // n_tp
    n_out = n_sp // 2

    me = lax.axis_index("sp")
    t = lax.axis_index("tp")
    outer = me // 2
    minor = me % 2
    partner = outer * 2 + 1 - minor
    tp_near = t + 1 - 2 * (t % 2)
    tp_far = (t + 2) % 4

    def peer(d):
        return ((outer + d) % n_out) * 2 + minor

    def origin(d):
        return (outer + n_out - d) % n_out

    loads = [
        pltpu.make_async_copy(src, dst, load_sem.at[i])
        for i, (src, dst) in enumerate(
            [
                (tok_hbm, tok), (wv_hbm, w_kv.at[:head]), (wk_hbm, w_kv.at[head:]),
                (wq_hbm, wq), (wo_hbm, wo),
                (qg_hbm, qg_ref), (kg_hbm, kg_ref),
            ]
        )
    ]
    for load in loads[5:] + loads[:3]:
        load.start()

    barrier = pltpu.get_barrier_semaphore()
    pl.semaphore_signal(barrier, inc=1, device_id={"sp": partner}, device_id_type=MESH)
    pl.semaphore_signal(barrier, inc=1, device_id={"tp": tp_near}, device_id_type=MESH)
    pl.semaphore_signal(barrier, inc=1, device_id={"tp": tp_far}, device_id_type=MESH)

    def greet(d, unused):
        pl.semaphore_signal(barrier, inc=1, device_id={"sp": peer(d)}, device_id_type=MESH)
        return unused

    lax.fori_loop(1, n_out, greet, 0)

    tabs = tables(me * rows, rows, heads, head // 4)
    key_tabs = tuple(x[:, :rows] for x in tabs)
    loads[5].wait()
    loads[6].wait()
    gain_q = column(qg_ref[...]) * (head ** -0.5)
    gain_k = column(kg_ref[...])

    loads[0].wait()
    loads[1].wait()
    loads[2].wait()
    loads[3].start()
    loads[4].start()
    raw_t = lax.dot_general(
        w_kv[...], tok[...], (((1,), (1,)), ((), ())), preferred_element_type=F32
    ).astype(BF16).astype(F32)
    keys_t = prepare(raw_t[head:], gain_k, key_tabs)
    kv_own[...] = jnp.concatenate([raw_t[:head], keys_t], axis=0).T.astype(BF16)

    piece = rows // 2

    def slot(i, k):
        return kvbuf.at[pl.ds(pl.multiple_of(i * rows + k * piece, 16), piece), :]

    def own(k):
        return kv_own.at[pl.ds(k * piece, piece), :]

    def to_partner(k):
        return pltpu.make_async_remote_copy(
            src_ref=own(k), dst_ref=slot(me, k), send_sem=send_sem.at[k], recv_sem=recv_sem.at[2 * me + k],
            device_id={"sp": partner}, device_id_type=MESH,
        )

    def to_peer(d, k):
        return pltpu.make_async_remote_copy(
            src_ref=own(k), dst_ref=slot(me, k), send_sem=send_sem.at[2 * d + k],
            recv_sem=recv_sem.at[2 * me + k],
            device_id={"sp": peer(d)}, device_id_type=MESH,
        )

    def forward(d, k):
        i = origin(d) * 2 + minor
        return pltpu.make_async_remote_copy(
            src_ref=slot(i, k), dst_ref=slot(i, k), send_sem=fwd_sem.at[2 * d + k],
            recv_sem=recv_sem.at[2 * i + k],
            device_id={"sp": partner}, device_id_type=MESH,
        )

    def land_piece(i, k):
        pltpu.make_async_remote_copy(
            src_ref=slot(i, k), dst_ref=slot(i, k), send_sem=send_sem.at[k],
            recv_sem=recv_sem.at[2 * i + k],
            device_id={"sp": partner}, device_id_type=MESH,
        ).wait_recv()

    def land(i):
        land_piece(i, 0)
        land_piece(i, 1)

    def held(i):
        return kvbuf[pl.ds(pl.multiple_of(i * rows, 16), rows), :]

    def arrival(i):
        land(i)
        return held(i)

    pl.semaphore_wait(barrier, n_out + 2)

    def send_peer(d, unused):
        to_peer(d, 0).start()
        to_peer(d, 1).start()
        return unused

    lax.fori_loop(1, n_out, send_peer, 0)
    to_partner(0).start()
    to_partner(1).start()

    loads[3].wait()
    raw_q = jnp.dot(tok[...], wq[...], preferred_element_type=F32).astype(BF16).astype(F32)
    stacked = jnp.concatenate([raw_q[:, h * head : (h + 1) * head] for h in range(heads)], axis=0)
    queries = prepare(stacked.T, gain_q, tabs)
    qpad[...] = jnp.concatenate([jnp.zeros_like(queries), queries], axis=0).astype(BF16)

    def attend(kv, state):
        scores = jnp.dot(kv, qpad[...], preferred_element_type=F32)
        top = jnp.max(scores, axis=0, keepdims=True)
        if state is not None:
            top = jnp.maximum(top, state[0])
        expos = jnp.exp(scores - top)
        total = jnp.sum(expos, axis=0, keepdims=True)
        summed = lax.dot_general(
            kv[:, :head], expos.astype(BF16), (((0,), (0,)), ((), ())), preferred_element_type=F32
        )
        if state is not None:
            shrink = jnp.exp(state[0] - top)
            total = total + state[1] * shrink
            summed = summed + state[2] * shrink
        return top, total, summed

    state = attend(kv_own[...], None)

    def take_direct(d, state):
        i = origin(d) * 2 + minor
        for k in range(2):
            land_piece(i, k)
            forward(d, k).start()
        return attend(held(i), state)

    def take_forwarded(d, state):
        return attend(arrival(origin(d) * 2 + 1 - minor), state)

    if n_out <= 8:
        ready = partner
        for d in range(1, n_out):
            i = origin(d) * 2 + minor
            for k in range(2):
                land_piece(i, k)
                forward(d, k).start()
            if d == 1:
                land(partner)
            state = attend(held(ready), state)
            ready = i
        state = attend(held(ready), state)
        for d in range(1, n_out):
            state = take_forwarded(d, state)
    else:
        state = attend(arrival(partner), state)
        state = lax.fori_loop(1, n_out, take_direct, state)
        state = lax.fori_loop(1, n_out, take_forwarded, state)
    top, total, summed = state

    result = (summed / total).T.astype(BF16)
    att[...] = jnp.concatenate([result[h * rows : (h + 1) * rows] for h in range(heads)], axis=1)

    def rows_of(j):
        return att[pl.ds(pl.multiple_of(j * part, 16), part), :]

    side, side_minor = t // 2, t % 2
    give = jnp.concatenate(
        [rows_of((1 - side) * 2 + 1 - side_minor), rows_of(side * 2 + 1 - side_minor)], axis=0
    )
    hold = jnp.concatenate([rows_of((1 - side) * 2 + side_minor), rows_of(t)], axis=0)

    loads[4].wait()

    def copy_a(c):
        return pltpu.make_async_remote_copy(
            src_ref=send_a.at[c], dst_ref=recv_a.at[c], send_sem=a_send.at[c], recv_sem=a_recv.at[c],
            device_id={"tp": tp_near}, device_id_type=MESH,
        )

    def copy_b(c):
        return pltpu.make_async_remote_copy(
            src_ref=send_b.at[c], dst_ref=recv_b.at[c], send_sem=b_send.at[c], recv_sem=b_recv.at[c],
            device_id={"tp": tp_far}, device_id_type=MESH,
        )

    for c in range(CHUNKS):
        cols = slice(c * chunk, (c + 1) * chunk)
        send_a[c] = jnp.dot(give, wo[:, cols], preferred_element_type=F32).astype(BF16)
        copy_a(c).start()
    for c in range(CHUNKS):
        cols = slice(c * chunk, (c + 1) * chunk)
        mine = jnp.dot(hold, wo[:, cols], preferred_element_type=F32)
        copy_a(c).wait_recv()
        mine = mine + recv_a[c].astype(F32)
        send_b[c] = mine[:part].astype(BF16)
        copy_b(c).start()
        keep[c] = mine[part:]

    logs = top + jnp.log(total)
    for h in range(heads):
        lse_ref[h : h + 1, :] = logs[:, h * rows : (h + 1) * rows]

    for c in range(CHUNKS):
        cols = slice(c * chunk, (c + 1) * chunk)
        copy_b(c).wait_recv()
        out_ref[:, cols] = (keep[c] + recv_b[c].astype(F32)).astype(BF16)

    def drain(d, unused):
        for k in range(2):
            to_peer(d, k).wait_send()
            forward(d, k).wait_send()
        return unused

    lax.fori_loop(1, n_out, drain, 0)
    to_partner(0).wait_send()
    to_partner(1).wait_send()
    for c in range(CHUNKS):
        copy_a(c).wait_send()
        copy_b(c).wait_send()


def solution(mesh):
    n_sp, n_tp = mesh.shape["sp"], mesh.shape["tp"]

    def shards(tokens, w_query, w_key, w_value, w_output, query_gain, key_gain):
        rows, depth = tokens.shape
        n_query, n_key = w_query.shape[1], w_key.shape[1]
        head = query_gain.shape[0]
        heads = n_query // head
        width = w_output.shape[1]
        part = rows // n_tp
        chunk = width // CHUNKS
        n_out = n_sp // 2
        hbm = pl.BlockSpec(memory_space=pl.ANY)
        vmem = pl.BlockSpec(memory_space=pltpu.VMEM)
        dma = pltpu.SemaphoreType.DMA
        def stay(x):
            return pltpu.with_memory_space_constraint(x, pltpu.HBM)

        return pl.pallas_call(
            functools.partial(kernel, n_sp, n_tp),
            out_shape=(
                jax.ShapeDtypeStruct((part, width), BF16),
                jax.ShapeDtypeStruct((heads, rows), F32),
            ),
            in_specs=[hbm] * 7,
            out_specs=(vmem, vmem),
            scratch_shapes=[
                pltpu.VMEM((rows, depth), BF16),
                pltpu.VMEM((depth, n_query), BF16),
                pltpu.VMEM((2 * n_key, depth), BF16),
                pltpu.VMEM((n_query, width), BF16),
                pltpu.VMEM((1, head), F32),
                pltpu.VMEM((1, head), F32),
                pltpu.VMEM((rows, 2 * head), BF16),
                pltpu.VMEM((n_sp * rows, 2 * head), BF16),
                pltpu.VMEM((2 * head, heads * rows), BF16),
                pltpu.VMEM((rows, n_query), BF16),
                pltpu.VMEM((CHUNKS, 2 * part, chunk), BF16),
                pltpu.VMEM((CHUNKS, 2 * part, chunk), BF16),
                pltpu.VMEM((CHUNKS, part, chunk), F32),
                pltpu.VMEM((CHUNKS, part, chunk), BF16),
                pltpu.VMEM((CHUNKS, part, chunk), BF16),
                dma((7,)),
                dma((2 * n_out,)),
                dma((2 * n_out,)),
                dma((2 * n_sp,)),
                dma((CHUNKS,)),
                dma((CHUNKS,)),
                dma((CHUNKS,)),
                dma((CHUNKS,)),
            ],
            compiler_params=pltpu.CompilerParams(collective_id=0, has_side_effects=True, vmem_limit_bytes=32 * 2**20),
            name="layer",
        )(
            stay(tokens), stay(w_query), stay(w_key.T), stay(w_value.T), stay(w_output),
            stay(query_gain[None, :]), stay(key_gain[None, :]),
        )

    placed = (P("sp", None), P(None, "tp"), P(None, "tp"), P(None, "tp"), P("tp", None), P(), P())
    return jax.shard_map(
        shards,
        mesh=mesh,
        in_specs=placed,
        out_specs=(P(("sp", "tp"), None), P("tp", "sp")),
        check_vma=False,
    )
```
